128 devices in a mesh: ra: 16 (over z, y), cb: 8 (over x, core).
Axes of the slice: x: 4, y: 4, z: 4, core: 2. Of those that a mesh axis runs over, the one named last changes fastest.
Arguments:
- tokens: bfloat16 [256, 3072], P(None, 'ra'), may hold values from -8 to 8, as said below
- first_gain: float32 [3072], P('ra'), may hold values from 0.1 to 1.9
- first_gate: float32 [3072, 8192], P('ra', 'cb'), may hold values from -0.109375 to 0.109375
- first_up: float32 [3072, 8192], P('ra', 'cb'), may hold values from -0.109375 to 0.109375
- first_down: float32 [8192, 3072], P('cb', 'ra'), may hold values from -0.0625 to 0.0625
- first_gate_scale: float32 [8192], P('cb'), may hold values from 0.5 to 2
- first_up_scale: float32 [8192], P('cb'), may hold values from 0.5 to 2
- first_down_scale: float32 [3072], P('ra'), may hold values from 0.5 to 2
- second_gain: float32 [3072], P('ra'), may hold values from 0.1 to 1.9
- second_gate: float32 [3072, 8192], P('ra', 'cb'), may hold values from -0.109375 to 0.109375
- second_up: float32 [3072, 8192], P('ra', 'cb'), may hold values from -0.109375 to 0.109375
- second_down: float32 [8192, 3072], P('cb', 'ra'), may hold values from -0.0625 to 0.0625
- second_gate_scale: float32 [8192], P('cb'), may hold values from 0.5 to 2
- second_up_scale: float32 [8192], P('cb'), may hold values from 0.5 to 2
- second_down_scale: float32 [3072], P('ra'), may hold values from 0.5 to 2
Outputs:
- mixed: bfloat16 [256, 3072], P(None, 'ra')
The draws below stay inside these ranges and needn't reach their ends.
Inputs may be any that keep to these rules, and one draw needn't show every extreme that they name: The features come in groups of 64 with different magnitudes, and tokens differ in magnitude.
All inputs are finite; a program needn't handle non-finite values.
Results may differ from the reference program's by a relative error of at most 0.0093.
Values may be sent and summed in bfloat16 or wider, within the bound.
No kernel may reach another device: no remote copies, remote signals or barrier semaphores. Data moves between devices by JAX's collectives and lax.ppermute only.
A program may use at most 64 MiB of HBM per device.

```python
import math
import jax
import jax.numpy as jnp
from jax import lax

D = 3072
FF = 8192
TOKENS = 256


def draw_tokens(key, part):
    base_key = jax.random.fold_in(key, 11)
    key_list = jax.random.split(base_key, 4)
    group_scale = jnp.exp(jax.random.uniform(key_list[0], (D // 64,), jnp.float32, math.log(0.1), 0.0))
    column_scale = jnp.repeat(group_scale, 64)
    row_scale = jnp.exp(jax.random.uniform(key_list[1], (TOKENS, 1), jnp.float32, math.log(0.5), math.log(2.0)))
    base_values = jnp.clip(jax.random.normal(key_list[3], (TOKENS, D), jnp.float32), -4.0, 4.0)
    return (base_values * column_scale[None, :] * row_scale).astype(jnp.bfloat16)


def block_levels(own_key, shape, cuts, smallest, largest):
    level = 1.0
    for position, parts in cuts:
        heights = jax.random.uniform(jax.random.fold_in(jax.random.fold_in(own_key, 6), position), (parts,), jnp.float32, smallest / len(cuts), largest / len(cuts))
        level = level * jnp.repeat(jnp.exp(heights), shape[position] // parts).reshape((-1,) + (1,) * (len(shape) - 1 - position))
    return level


def scatter_about(stream_key, shape, deviation, most, cuts=(), dtype=jnp.bfloat16):
    loudness = block_levels(stream_key, shape, cuts, -0.22, 0.18) if cuts else 1.0
    array = jax.random.normal(stream_key, shape, jnp.float32) * deviation * loudness
    return jnp.minimum(jnp.maximum(array, -most), most).astype(dtype)


def setup_inputs(seed: int = 0) -> dict:
    arg_keys = jax.random.split(jax.random.key(seed), 16)
    return {
        "tokens": draw_tokens(jax.random.fold_in(arg_keys[15], 71), 0),
        "first_gain": jnp.clip(1.0 + 0.18 * jax.random.normal(arg_keys[1], (D,), jnp.float32), 0.1, 1.9),
        "first_gate": scatter_about(arg_keys[2], (D, FF), D ** -0.5, 0.109375, ((0, 16), (1, 8)), jnp.float32),
        "first_up": scatter_about(arg_keys[3], (D, FF), D ** -0.5, 0.109375, ((0, 16), (1, 8)), jnp.float32),
        "first_down": scatter_about(arg_keys[4], (FF, D), FF ** -0.5, 0.0625, ((0, 8), (1, 16)), jnp.float32),
        "first_gate_scale": jnp.clip(jnp.exp(math.log(2.0) - 1.3862944 * jax.random.uniform(arg_keys[5], (FF,), jnp.float32) ** block_levels(arg_keys[5], (FF,), ((0, 8),), -0.2, 0.2)), 0.5, 2.0),
        "first_up_scale": jnp.clip(jnp.exp(math.log(2.0) - 1.3862944 * jax.random.uniform(arg_keys[6], (FF,), jnp.float32) ** block_levels(arg_keys[6], (FF,), ((0, 8),), -0.2, 0.2)), 0.5, 2.0),
        "first_down_scale": jnp.clip(jnp.exp(math.log(2.0) - 1.3862944 * jax.random.uniform(arg_keys[7], (D,), jnp.float32) ** block_levels(arg_keys[7], (D,), ((0, 16),), -0.2, 0.2)), 0.5, 2.0),
        "second_gain": jnp.clip(1.0 + 0.18 * jax.random.normal(arg_keys[8], (D,), jnp.float32), 0.1, 1.9),
        "second_gate": scatter_about(arg_keys[9], (D, FF), D ** -0.5, 0.109375, ((0, 16), (1, 8)), jnp.float32),
        "second_up": scatter_about(arg_keys[10], (D, FF), D ** -0.5, 0.109375, ((0, 16), (1, 8)), jnp.float32),
        "second_down": scatter_about(arg_keys[11], (FF, D), FF ** -0.5, 0.0625, ((0, 8), (1, 16)), jnp.float32),
        "second_gate_scale": jnp.clip(jnp.exp(math.log(2.0) - 1.3862944 * jax.random.uniform(arg_keys[12], (FF,), jnp.float32) ** block_levels(arg_keys[12], (FF,), ((0, 8),), -0.2, 0.2)), 0.5, 2.0),
        "second_up_scale": jnp.clip(jnp.exp(math.log(2.0) - 1.3862944 * jax.random.uniform(arg_keys[13], (FF,), jnp.float32) ** block_levels(arg_keys[13], (FF,), ((0, 8),), -0.2, 0.2)), 0.5, 2.0),
        "second_down_scale": jnp.clip(jnp.exp(math.log(2.0) - 1.3862944 * jax.random.uniform(arg_keys[14], (D,), jnp.float32) ** block_levels(arg_keys[14], (D,), ((0, 16),), -0.2, 0.2)), 0.5, 2.0),
    }


def half_step(stream_in, gain, w_gate, w_up, w_down, gate_scale, up_scale, down_scale):
    stream = stream_in.astype(jnp.float32)
    msq = lax.optimization_barrier(jnp.mean(stream * stream, axis=1))
    shaped = (stream * gain[None, :]).astype(jnp.bfloat16)
    inverse = lax.rsqrt(msq + 1e-06)[:, None]
    gate_full = inverse * gate_scale[None, :] * jnp.dot(shaped, w_gate.astype(jnp.bfloat16), preferred_element_type=jnp.float32)
    up_full = inverse * up_scale[None, :] * jnp.dot(shaped, w_up.astype(jnp.bfloat16), preferred_element_type=jnp.float32)
    hidden = (jax.nn.silu(gate_full) * up_full).astype(jnp.bfloat16)
    down_full = down_scale[None, :] * jnp.dot(hidden, w_down.astype(jnp.bfloat16), preferred_element_type=jnp.float32)
    return (stream + 0.5 * down_full).astype(jnp.bfloat16)

def reference(tokens, first_gain, first_gate, first_up, first_down, first_gate_scale, first_up_scale, first_down_scale, second_gain, second_gate, second_up, second_down, second_gate_scale, second_up_scale, second_down_scale):
    middle = half_step(tokens, first_gain, first_gate, first_up, first_down, first_gate_scale, first_up_scale, first_down_scale)
    return half_step(middle, second_gain, second_gate, second_up, second_down, second_gate_scale, second_up_scale, second_down_scale)
```

```python
import jax
import jax.numpy as jnp
from jax import lax
from jax.sharding import PartitionSpec as P

D = 3072
PARTS = 1
BF16 = jnp.bfloat16
F32 = jnp.float32


def swap(tiles, axis):
    return lax.all_to_all(tiles, axis, 0, 0, tiled=True)


def to_all(shard, axis):
    peers = lax.axis_size(axis)
    return swap(jnp.broadcast_to(shard[None], (peers, *shard.shape)), axis)


def products(stream, gain, w_gate, w_up):
    squares = jnp.sum(stream * stream, axis=1)
    high = lax.reduce_precision(squares, 8, 7)
    low = squares - high
    shaped = (stream * gain[None, :]).astype(BF16)
    gate = jnp.dot(shaped, w_gate, preferred_element_type=F32).astype(BF16)
    up = jnp.dot(shaped, w_up, preferred_element_type=F32).astype(BF16)
    lane = lax.broadcasted_iota(jnp.int32, (stream.shape[0], 128), 1)
    extra = jnp.where(lane == 0, high[:, None], jnp.where(lane == 1, low[:, None], 0.0)).astype(BF16)
    both = jnp.concatenate([gate, up, extra], axis=1)
    peers = lax.axis_size("ra")
    return both.reshape(peers, -1, both.shape[1])


def hidden_of(tiles, gate_scale, up_scale):
    total = jnp.sum(tiles.astype(F32), axis=0)
    units = gate_scale.shape[0]
    squares = total[:, 2 * units] + total[:, 2 * units + 1]
    inverse = lax.rsqrt(squares / D + 1e-06)[:, None]
    gate = inverse * gate_scale[None, :] * total[:, :units]
    up = inverse * up_scale[None, :] * total[:, units : 2 * units]
    return (jax.nn.silu(gate) * up).astype(BF16)


def half_step(streams, gain, w_gate, w_up, w_down, gate_scale, up_scale, down_scale):
    w_gate, w_up, w_down = (w.astype(BF16) for w in (w_gate, w_up, w_down))
    scale = 0.5 * down_scale
    results = []
    for stream_in in streams:
        stream = stream_in.astype(F32)
        tiles = swap(products(stream, gain, w_gate, w_up), "ra")
        hidden = to_all(hidden_of(tiles, gate_scale, up_scale), "ra")
        hidden = hidden.reshape(-1, hidden.shape[-1])
        down = jnp.dot(hidden, w_down, preferred_element_type=F32).astype(BF16)
        total = jnp.sum(to_all(down, "cb").astype(F32), axis=0)
        results.append((stream + scale[None, :] * total).astype(BF16))
    return results


def body(tokens, *rest):
    streams = jnp.split(tokens, PARTS, axis=0)
    streams = half_step(streams, *rest[:7])
    streams = half_step(streams, *rest[7:])
    return jnp.concatenate(streams, axis=0)


def solution(mesh):
    one = (P("ra"), P("ra", "cb"), P("ra", "cb"), P("cb", "ra"), P("cb"), P("cb"), P("ra"))
    return jax.shard_map(
        body, mesh=mesh, in_specs=(P(None, "ra"), *one, *one), out_specs=P(None, "ra"), check_vma=False
    )
```

```python
import jax
import jax.numpy as jnp
from jax import lax
from jax.sharding import PartitionSpec as P

D = 3072
BF16 = jnp.bfloat16
F32 = jnp.float32


def rounded(x):
    return lax.reduce_precision(x, 8, 7)


def swap(tiles, axis):
    return lax.all_to_all(tiles, axis, 0, 0, tiled=True)


def to_all(shard, axis):
    peers = lax.axis_size(axis)
    return swap(jnp.broadcast_to(shard[None], (peers, *shard.shape)), axis)


def sum_over_cb(part):
    n = lax.axis_size("cb")

    def moved(value, pairs):
        return lax.ppermute(value.astype(BF16), "cb", pairs).astype(F32)

    part = rounded(part)
    chip = rounded(part + moved(part, [(i, i ^ 1) for i in range(n)]))
    if n == 2:
        return chip
    before = moved(chip, [(i, (i + 2) % n) for i in range(n)])
    after = moved(chip, [(i, (i - 2) % n) for i in range(n)])
    across = moved(chip, [(i, (i + 4) % n) for i in range(n)])
    return (chip + across) + (before + after)


def products(stream, gain, w_gate, w_up):
    squares = jnp.sum(stream * stream, axis=1)
    high = rounded(squares)
    low = squares - high
    shaped = (stream * gain[None, :]).astype(BF16)
    gate = jnp.dot(shaped, w_gate, preferred_element_type=F32).astype(BF16)
    up = jnp.dot(shaped, w_up, preferred_element_type=F32).astype(BF16)
    lane = lax.broadcasted_iota(jnp.int32, (stream.shape[0], 128), 1)
    extra = jnp.where(lane == 0, high[:, None], jnp.where(lane == 1, low[:, None], 0.0)).astype(BF16)
    both = jnp.concatenate([gate, up, extra], axis=1)
    return both.reshape(lax.axis_size("ra"), -1, both.shape[1])


def hidden_of(tiles, gate_scale, up_scale):
    total = jnp.sum(tiles.astype(F32), axis=0)
    units = gate_scale.shape[0]
    squares = total[:, 2 * units] + total[:, 2 * units + 1]
    inverse = lax.rsqrt(squares / D + 1e-06)[:, None]
    gate = inverse * gate_scale[None, :] * total[:, :units]
    up = inverse * up_scale[None, :] * total[:, units : 2 * units]
    return (jax.nn.silu(gate) * up).astype(BF16)


def half_step(stream_in, gain, w_gate, w_up, w_down, gate_scale, up_scale, down_scale):
    w_gate, w_up, w_down = (w.astype(BF16) for w in (w_gate, w_up, w_down))
    stream = stream_in.astype(F32)
    tiles = swap(products(stream, gain, w_gate, w_up), "ra")
    hidden = to_all(hidden_of(tiles, gate_scale, up_scale), "ra")
    hidden = hidden.reshape(-1, hidden.shape[-1])
    down = sum_over_cb(jnp.dot(hidden, w_down, preferred_element_type=F32))
    return (stream + 0.5 * down_scale[None, :] * down).astype(BF16)


def body(tokens, *rest):
    return half_step(half_step(tokens, *rest[:7]), *rest[7:])


def solution(mesh):
    one = (P("ra"), P("ra", "cb"), P("ra", "cb"), P("cb", "ra"), P("cb"), P("cb"), P("ra"))
    return jax.shard_map(
        body, mesh=mesh, in_specs=(P(None, "ra"), *one, *one), out_specs=P(None, "ra"), check_vma=False
    )
```

```python
import jax
import jax.numpy as jnp
from jax import lax
from jax.experimental import pallas as pl
from jax.experimental.pallas import tpu as pltpu
from jax.sharding import PartitionSpec as P

D = 3072
BF16 = jnp.bfloat16
F32 = jnp.float32


def rounded(x):
    return lax.reduce_precision(x, 8, 7)


def swap(tiles, axis):
    return lax.all_to_all(tiles, axis, 0, 0, tiled=True)


def sum_over_cb(part):
    n = lax.axis_size("cb")

    def moved(value, pairs):
        return lax.ppermute(value.astype(BF16), "cb", pairs).astype(F32)

    part = rounded(part)
    chip = rounded(part + moved(part, [(i, i ^ 1) for i in range(n)]))
    if n == 2:
        return chip
    before = moved(chip, [(i, (i + 2) % n) for i in range(n)])
    after = moved(chip, [(i, (i - 2) % n) for i in range(n)])
    across = moved(chip, [(i, (i + 4) % n) for i in range(n)])
    return (chip + across) + (before + after)


CHUNKS = 4
VMEM = pl.BlockSpec(memory_space=pltpu.VMEM)
HBM = pl.BlockSpec(memory_space=pltpu.HBM)


def write_squares(stream, out_ref, start):
    squares = jnp.sum(stream * stream, axis=1, keepdims=True)
    high = squares.astype(BF16).astype(F32)
    lane = lax.broadcasted_iota(jnp.int32, (stream.shape[0], 128), 1)
    extra = jnp.where(lane == 0, high, jnp.where(lane == 1, squares - high, 0.0))
    out_ref[:, start:] = extra.astype(BF16)


def fetching_kernel(
    stream_ref, gain_ref, gate_ref, up_ref, gate_scale_ref, up_scale_ref, out_ref, scales_ref, stream_held, gain_held, held, sems, small_sems
):
    units = gate_ref.shape[1]
    wide = 2 * units // CHUNKS
    small = [
        pltpu.make_async_copy(ref, held_ref, small_sems.at[k])
        for k, (ref, held_ref) in enumerate(
            (
                (stream_ref, stream_held),
                (gain_ref, gain_held),
                (gate_scale_ref, scales_ref.at[0]),
                (up_scale_ref, scales_ref.at[1]),
            )
        )
    ]
    for copy in small[:2]:
        copy.start()
    copies = []
    for k in range(CHUNKS):
        ref, at = (gate_ref, k * wide) if k * wide < units else (up_ref, k * wide - units)
        copies.append(pltpu.make_async_copy(ref.at[:, pl.ds(at, wide)], held.at[k], sems.at[k]))
        copies[-1].start()
    for copy in small[2:]:
        copy.start()
    small[0].wait()
    stream = stream_held[...].astype(F32).T
    write_squares(stream, out_ref, 2 * units)
    small[1].wait()
    shaped = (stream * gain_held[...]).astype(BF16)
    for k, copy in enumerate(copies):
        copy.wait()
        part = jnp.dot(shaped, held[k].astype(BF16), preferred_element_type=F32)
        out_ref[:, k * wide : (k + 1) * wide] = part.astype(BF16)
    for copy in small[2:]:
        copy.wait()


def products_kernel(stream_ref, gain_ref, gate_ref, up_ref, gate_scale_ref, up_scale_ref, out_ref, scales_ref):
    units = gate_ref.shape[1]
    wide = 2 * units // CHUNKS
    scales_ref[0] = gate_scale_ref[...]
    scales_ref[1] = up_scale_ref[...]
    stream = stream_ref[...].astype(F32).T
    write_squares(stream, out_ref, 2 * units)
    shaped = (stream * gain_ref[...]).astype(BF16)
    for k in range(CHUNKS):
        ref, at = (gate_ref, k * wide) if k * wide < units else (up_ref, k * wide - units)
        part = jnp.dot(shaped, ref[:, at : at + wide].astype(BF16), preferred_element_type=F32)
        out_ref[:, k * wide : (k + 1) * wide] = part.astype(BF16)


def products(fetch, stream, gain, w_gate, w_up, gate_scale, up_scale):
    tokens, features = stream.shape
    units = w_gate.shape[1]
    scratch = [
        pltpu.VMEM((features, tokens), BF16),
        pltpu.VMEM((1, features), F32),
        pltpu.VMEM((CHUNKS, features, 2 * units // CHUNKS), F32),
        pltpu.SemaphoreType.DMA((CHUNKS,)),
        pltpu.SemaphoreType.DMA((4,)),
    ]
    operands = [stream.T, gain[None, :], w_gate, w_up, gate_scale[None, :], up_scale[None, :]]
    if fetch:
        operands = [pltpu.with_memory_space_constraint(x, pltpu.HBM) for x in operands]
    both, scales = pl.pallas_call(
        fetching_kernel if fetch else products_kernel,
        out_shape=(
            jax.ShapeDtypeStruct((tokens, 2 * units + 128), BF16),
            jax.ShapeDtypeStruct((2, 1, units), F32),
        ),
        in_specs=[HBM if fetch else VMEM] * 6,
        out_specs=(VMEM, VMEM),
        scratch_shapes=scratch if fetch else [],
        compiler_params=pltpu.CompilerParams(vmem_limit_bytes=12 << 20),
        cost_estimate=pl.CostEstimate(
            flops=4 * tokens * features * units, bytes_accessed=8 * features * units, transcendentals=0
        ),
    )(*operands)
    return both.reshape(lax.axis_size("ra"), -1, both.shape[1]), scales


def hidden_kernel(tiles_ref, scales_ref, out_ref):
    units = scales_ref.shape[2]
    total = jnp.sum(tiles_ref[:, :, 2 * units :].astype(F32), axis=0)
    inverse = lax.rsqrt((total[:, 0:1] + total[:, 1:2]) / D + 1e-06)
    gate = inverse * scales_ref[0] * jnp.sum(tiles_ref[:, :, :units].astype(F32), axis=0)
    up = inverse * scales_ref[1] * jnp.sum(tiles_ref[:, :, units : 2 * units].astype(F32), axis=0)
    hidden = (gate / (1.0 + jnp.exp(-gate)) * up).astype(BF16)
    for k in range(out_ref.shape[0]):
        out_ref[k] = hidden


def hidden_of(tiles, scales):
    peers, rows, _ = tiles.shape
    units = scales.shape[2]
    return pl.pallas_call(
        hidden_kernel,
        out_shape=jax.ShapeDtypeStruct((peers, rows, units), BF16),
        in_specs=[VMEM, VMEM],
        out_specs=VMEM,
        compiler_params=pltpu.CompilerParams(vmem_limit_bytes=12 << 20),
        cost_estimate=pl.CostEstimate(
            flops=2 * tiles.size, bytes_accessed=4 * tiles.size, transcendentals=rows * units
        ),
    )(tiles, scales)


def half_step(fetch, stream, gain, w_gate, w_up, w_down, gate_scale, up_scale, down_scale):
    part, scales = products(fetch, stream, gain, w_gate, w_up, gate_scale, up_scale)
    hidden = swap(hidden_of(swap(part, "ra"), scales), "ra")
    hidden = hidden.reshape(-1, hidden.shape[-1])
    down = sum_over_cb(jnp.dot(hidden, w_down.astype(BF16), preferred_element_type=F32))
    return (stream.astype(F32) + 0.5 * down_scale[None, :] * down).astype(BF16)


def body(tokens, *rest):
    return half_step(False, half_step(True, tokens, *rest[:7]), *rest[7:])


def solution(mesh):
    one = (P("ra"), P("ra", "cb"), P("ra", "cb"), P("cb", "ra"), P("cb"), P("cb"), P("ra"))
    return jax.shard_map(
        body, mesh=mesh, in_specs=(P(None, "ra"), *one, *one), out_specs=P(None, "ra"), check_vma=False
    )
```

```python
import jax
import jax.numpy as jnp
from jax import lax
from jax.experimental import pallas as pl
from jax.experimental.pallas import tpu as pltpu
from jax.sharding import PartitionSpec as P

D = 3072
SIDE = 4
CHUNKS = 4
BF16 = jnp.bfloat16
F32 = jnp.float32
VMEM = pl.BlockSpec(memory_space=pltpu.VMEM)
HBM = pl.BlockSpec(memory_space=pltpu.HBM)
PARAMS = pltpu.CompilerParams(vmem_limit_bytes=12 << 20)


def rounded(x):
    return lax.reduce_precision(x, 8, 7)


def place_in_f():
    ra, cb = lax.axis_index("ra"), lax.axis_index("cb")
    return jnp.where(cb % 2 == 0, ra // SIDE, ra % SIDE)


def pairs_of(shift, along_f):
    pairs = []
    for z in range(SIDE):
        for y in range(SIDE):
            for cb in range(8):
                if (cb % 2 == 0) == along_f:
                    to = ((z + shift) % SIDE, y)
                else:
                    to = (z, (y + shift) % SIDE)
                pairs.append(((z * SIDE + y) * 8 + cb, (to[0] * SIDE + to[1]) * 8 + cb))
    return pairs


def moved(x, shift, along_f):
    return lax.ppermute(x, ("ra", "cb"), pairs_of(shift, along_f))


def sum_over_cb(part):
    n = lax.axis_size("cb")

    def shifted(value, pairs):
        return lax.ppermute(value.astype(BF16), "cb", pairs).astype(F32)

    chip = rounded(part.astype(F32) + shifted(part, [(i, i ^ 1) for i in range(n)]))
    across, before, after = (shifted(chip, [(i, (i + 2 * k) % n) for i in range(n)]) for k in (2, 1, 3))
    return (chip + across) + (before + after)


def squares_tile(high_low):
    high = high_low.astype(BF16).astype(F32)
    lane = lax.broadcasted_iota(jnp.int32, (high_low.shape[0], 128), 1)
    return jnp.where(lane == 0, high, jnp.where(lane == 1, high_low - high, 0.0)).astype(BF16)


def turned_rows(stream_ref, turned):
    tokens = stream_ref.shape[1]
    rows = tokens // SIDE
    turned[0] = stream_ref[...].astype(F32).T
    place = place_in_f()
    for k in range(SIDE):
        at = pl.multiple_of((place + k) % SIDE * rows, rows)
        turned[1, k * rows : (k + 1) * rows] = turned[0, pl.ds(at, rows)]
    return turned[1]


def write_products(stream, gain, weights_of, units, out_refs):
    rows = stream.shape[0] // SIDE
    tile = squares_tile(jnp.sum(stream * stream, axis=1, keepdims=True))
    for k, out_ref in enumerate(out_refs):
        out_ref[:, 2 * units :] = tile[k * rows : (k + 1) * rows]
    shaped = (stream * gain).astype(BF16)
    wide = 2 * units // CHUNKS
    for c in range(CHUNKS):
        part = jnp.dot(shaped, weights_of(c).astype(BF16), preferred_element_type=F32).astype(BF16)
        for k, out_ref in enumerate(out_refs):
            out_ref[:, c * wide : (c + 1) * wide] = part[k * rows : (k + 1) * rows]


def fetching_kernel(stream_ref, gain_ref, gate_ref, up_ref, gate_scale_ref, up_scale_ref, *refs):
    out_refs, (scales_ref, turned, stream_held, gain_held, held, sems, small_sems) = refs[:SIDE], refs[SIDE:]
    units = gate_ref.shape[1]
    wide = 2 * units // CHUNKS
    small = [
        pltpu.make_async_copy(ref, held_ref, small_sems.at[k])
        for k, (ref, held_ref) in enumerate(
            (
                (stream_ref, stream_held),
                (gain_ref, gain_held),
                (gate_scale_ref, scales_ref.at[0]),
                (up_scale_ref, scales_ref.at[1]),
            )
        )
    ]
    for copy in small[:2]:
        copy.start()
    copies = []
    for k in range(CHUNKS):
        ref, at = (gate_ref, k * wide) if k * wide < units else (up_ref, k * wide - units)
        copies.append(pltpu.make_async_copy(ref.at[:, pl.ds(at, wide)], held.at[k], sems.at[k]))
        copies[-1].start()
    for copy in small[2:]:
        copy.start()

    def weights_of(c):
        copies[c].wait()
        return held[c]

    small[0].wait()
    stream = turned_rows(stream_held, turned)
    small[1].wait()
    write_products(stream, gain_held[...], weights_of, units, out_refs)
    for copy in small[2:]:
        copy.wait()


def products_kernel(stream_ref, gain_ref, gate_ref, up_ref, gate_scale_ref, up_scale_ref, *refs):
    out_refs, (scales_ref, turned) = refs[:SIDE], refs[SIDE:]
    units = gate_ref.shape[1]
    wide = 2 * units // CHUNKS

    def weights_of(c):
        ref, at = (gate_ref, c * wide) if c * wide < units else (up_ref, c * wide - units)
        return ref[:, at : at + wide]

    scales_ref[0] = gate_scale_ref[...]
    scales_ref[1] = up_scale_ref[...]
    write_products(turned_rows(stream_ref, turned), gain_ref[...], weights_of, units, out_refs)


def products(fetch, stream, gain, w_gate, w_up, gate_scale, up_scale):
    features, tokens = stream.shape
    units = w_gate.shape[1]
    scratch = [
        pltpu.VMEM((2, tokens, features), F32),
        pltpu.VMEM((features, tokens), BF16),
        pltpu.VMEM((1, features), F32),
        pltpu.VMEM((CHUNKS, features, 2 * units // CHUNKS), F32),
        pltpu.SemaphoreType.DMA((CHUNKS,)),
        pltpu.SemaphoreType.DMA((4,)),
    ]
    operands = [stream, gain[None, :], w_gate, w_up, gate_scale[None, :], up_scale[None, :]]
    if fetch:
        operands = [pltpu.with_memory_space_constraint(x, pltpu.HBM) for x in operands]
    block = jax.ShapeDtypeStruct((tokens // SIDE, 2 * units + 128), BF16)
    *blocks, scales = pl.pallas_call(
        fetching_kernel if fetch else products_kernel,
        out_shape=(*[block] * SIDE, jax.ShapeDtypeStruct((2, 1, units), F32)),
        in_specs=[HBM if fetch else VMEM] * 6,
        out_specs=(VMEM,) * (SIDE + 1),
        scratch_shapes=scratch if fetch else scratch[:1],
        compiler_params=PARAMS,
        cost_estimate=pl.CostEstimate(
            flops=4 * tokens * features * units, bytes_accessed=8 * features * units, transcendentals=0
        ),
    )(*operands)
    return blocks, scales


def add_kernel(*refs):
    *in_refs, out_ref = refs
    end = out_ref.shape[1] - 128
    total = sum(ref[...].astype(F32) for ref in in_refs[1:]) + in_refs[0][...].astype(F32)
    out_ref[:, :end] = total[:, :end].astype(BF16)
    out_ref[:, end:] = squares_tile(total[:, end : end + 1] + total[:, end + 1 : end + 2])


def hidden_kernel(*refs):
    *in_refs, scales_ref, out_ref = refs
    units = scales_ref.shape[2]
    total = sum(ref[...].astype(F32) for ref in in_refs[1:]) + in_refs[0][...].astype(F32)
    squares = total[:, 2 * units : 2 * units + 1] + total[:, 2 * units + 1 : 2 * units + 2]
    inverse = lax.rsqrt(squares / D + 1e-06)
    gate = inverse * scales_ref[0] * total[:, :units]
    up = inverse * scales_ref[1] * total[:, units : 2 * units]
    out_ref[...] = (gate / (1.0 + jnp.exp(-gate)) * up).astype(BF16)


def down_kernel(*refs):
    *in_refs, w_ref, out_ref, hidden = refs
    rows = in_refs[0].shape[0]
    place = place_in_f()
    for k, ref in enumerate(in_refs):
        at = pl.multiple_of((place + k) % SIDE * rows, rows)
        hidden[pl.ds(at, rows)] = ref[...]
    out_ref[...] = lax.dot_general(
        w_ref[...].astype(BF16), hidden[...], (((1,), (1,)), ((), ())), preferred_element_type=F32
    ).astype(BF16)


def call(kernel, shape, *operands, scratch=(), flops=0):
    return pl.pallas_call(
        kernel,
        out_shape=jax.ShapeDtypeStruct(shape, BF16),
        in_specs=[VMEM] * len(operands),
        out_specs=VMEM,
        scratch_shapes=scratch,
        compiler_params=PARAMS,
        cost_estimate=pl.CostEstimate(
            flops=flops or 8 * operands[0].size,
            bytes_accessed=sum(x.size * x.dtype.itemsize for x in operands),
            transcendentals=0,
        ),
    )(*operands)


def half_step(fetch, stream, gain, w_gate, w_up, w_down, gate_scale, up_scale, down_scale):
    blocks, scales = products(fetch, stream, gain, w_gate, w_up, gate_scale, up_scale)
    mine = call(add_kernel, blocks[0].shape, blocks[0], *(moved(blocks[k], k, True) for k in (2, 1, 3)))
    peers = [moved(mine, k, False) for k in (2, 1, 3)]
    hidden = call(hidden_kernel, (mine.shape[0], w_gate.shape[1]), mine, *peers, scales)
    behind = {k: moved(hidden, k, True) for k in (2, 1, 3)}
    units, features = w_down.shape
    tokens = stream.shape[1]
    down = call(
        down_kernel,
        (features, tokens),
        hidden,
        behind[3],
        behind[2],
        behind[1],
        w_down.T,
        scratch=[pltpu.VMEM((tokens, units), BF16)],
        flops=2 * tokens * units * features,
    )
    return (stream.astype(F32) + 0.5 * down_scale[:, None] * sum_over_cb(down)).astype(BF16)


def body(tokens, *rest):
    return half_step(False, half_step(True, tokens.T, *rest[:7]), *rest[7:]).T


def solution(mesh):
    one = (P("ra"), P("ra", "cb"), P("ra", "cb"), P("cb", "ra"), P("cb"), P("cb"), P("ra"))
    return jax.shard_map(
        body, mesh=mesh, in_specs=(P(None, "ra"), *one, *one), out_specs=P(None, "ra"), check_vma=False
    )
```

```python
import jax
import jax.numpy as jnp
from jax import lax
from jax.experimental import pallas as pl
from jax.experimental.pallas import tpu as pltpu
from jax.sharding import PartitionSpec as P

D = 3072
SIDE = 4
CHUNKS = 4
ORDER = (2, 1, 3)
X_ORDER = (2, 1, 3)
BF16 = jnp.bfloat16
F32 = jnp.float32
VMEM = pl.BlockSpec(memory_space=pltpu.VMEM)
HBM = pl.BlockSpec(memory_space=pltpu.HBM)
PARAMS = pltpu.CompilerParams(vmem_limit_bytes=12 << 20)


def rounded(x):
    return lax.reduce_precision(x, 8, 7)


def place_in_f():
    ra, cb = lax.axis_index("ra"), lax.axis_index("cb")
    return jnp.where(cb % 2 == 0, ra // SIDE, ra % SIDE)


def pairs_of(k, along_f):
    pairs = []
    for z in range(SIDE):
        for y in range(SIDE):
            for cb in range(8):
                if (cb % 2 == 0) == along_f:
                    to = (z ^ k, y)
                else:
                    to = (z, y ^ k)
                pairs.append(((z * SIDE + y) * 8 + cb, (to[0] * SIDE + to[1]) * 8 + cb))
    return pairs


def swapped(x, k, along_f):
    return lax.ppermute(x, ("ra", "cb"), pairs_of(k, along_f))


def sum_over_cb(part):
    n = lax.axis_size("cb")

    def shifted(value, pairs):
        return lax.ppermute(value.astype(BF16), "cb", pairs).astype(F32)

    chip = rounded(part.astype(F32) + shifted(part, [(i, i ^ 1) for i in range(n)]))
    others = {k: shifted(chip, [(i, i ^ 2 * k) for i in range(n)]) for k in X_ORDER}
    return (chip + others[2]) + (others[1] + others[3])


def packed_squares(squares):
    high = squares.astype(BF16).astype(F32)
    low = squares - high
    lane = lax.broadcasted_iota(jnp.int32, (8, 128), 1)
    tile = jnp.zeros((8, 128), F32)
    for k in range(squares.shape[0] // 8):
        tile = jnp.where(lane == 2 * k, high[8 * k : 8 * k + 8], tile)
        tile = jnp.where(lane == 2 * k + 1, low[8 * k : 8 * k + 8], tile)
    return tile.astype(BF16)


def whole_squares(tile):
    return tile + pltpu.roll(tile, 127, 1)


def turned_rows(stream_ref, turned):
    tokens = stream_ref.shape[1]
    rows = tokens // SIDE
    turned[0] = stream_ref[...].astype(F32).T
    place = place_in_f()
    for k in range(SIDE):
        at = pl.multiple_of((place ^ k) * rows, rows)
        turned[1, k * rows : (k + 1) * rows] = turned[0, pl.ds(at, rows)]
    return turned[1]


def write_products(stream, gain, weights_of, units, out_refs):
    rows = stream.shape[0] // SIDE
    squares = jnp.sum(stream * stream, axis=1, keepdims=True)
    for k, out_ref in enumerate(out_refs):
        out_ref[2 * units // 128 * rows :] = packed_squares(squares[k * rows : (k + 1) * rows])
    shaped = (stream * gain).astype(BF16)
    wide = 2 * units // CHUNKS
    for c in range(CHUNKS):
        part = jnp.dot(shaped, weights_of(c).astype(BF16), preferred_element_type=F32).astype(BF16)
        for k, out_ref in enumerate(out_refs):
            for n in range(wide // 128):
                at = (c * wide // 128 + n) * rows
                out_ref[at : at + rows] = part[k * rows : (k + 1) * rows, n * 128 : (n + 1) * 128]


def fetching_kernel(stream_ref, gain_ref, gate_ref, up_ref, *refs):
    small_refs, refs = refs[:5], refs[5:]
    out_refs, (scales_ref, later_scales_ref, later_gain_ref), refs = refs[:SIDE], refs[SIDE : SIDE + 3], refs[SIDE + 3 :]
    turned, stream_held, gain_held, held, sems, small_sems = refs
    units = gate_ref.shape[1]
    wide = 2 * units // CHUNKS
    targets = (
        stream_held,
        gain_held,
        scales_ref.at[0],
        scales_ref.at[1],
        later_scales_ref.at[0],
        later_scales_ref.at[1],
        later_gain_ref,
    )
    small = [
        pltpu.make_async_copy(ref, target, small_sems.at[k])
        for k, (ref, target) in enumerate(zip((stream_ref, gain_ref, *small_refs), targets, strict=True))
    ]
    for copy in small[:2]:
        copy.start()
    copies = []
    for k in range(CHUNKS):
        ref, at = (gate_ref, k * wide) if k * wide < units else (up_ref, k * wide - units)
        copies.append(pltpu.make_async_copy(ref.at[:, pl.ds(at, wide)], held.at[k], sems.at[k]))
        copies[-1].start()
    for copy in small[2:]:
        copy.start()

    def weights_of(c):
        copies[c].wait()
        return held[c]

    small[0].wait()
    stream = turned_rows(stream_held, turned)
    small[1].wait()
    write_products(stream, gain_held[...], weights_of, units, out_refs)
    for copy in small[2:]:
        copy.wait()


def products_kernel(stream_ref, gain_ref, gate_ref, up_ref, *refs):
    *out_refs, turned = refs
    units = gate_ref.shape[1]
    wide = 2 * units // CHUNKS

    def weights_of(c):
        ref, at = (gate_ref, c * wide) if c * wide < units else (up_ref, c * wide - units)
        return ref[:, at : at + wide]

    write_products(turned_rows(stream_ref, turned), gain_ref[...], weights_of, units, out_refs)


def products(stream, gain, w_gate, w_up, *small):
    features, tokens = stream.shape
    units = w_gate.shape[1]
    scratch = [
        pltpu.VMEM((2, tokens, features), F32),
        pltpu.VMEM((features, tokens), BF16),
        pltpu.VMEM((1, features), F32),
        pltpu.VMEM((CHUNKS, features, 2 * units // CHUNKS), F32),
        pltpu.SemaphoreType.DMA((CHUNKS,)),
        pltpu.SemaphoreType.DMA((7,)),
    ]
    operands = [stream, gain, w_gate, w_up, *small]
    rows = tokens // SIDE
    outs = [jax.ShapeDtypeStruct((2 * units // 128 * rows + 8, 128), BF16)] * SIDE
    if small:
        operands = [pltpu.with_memory_space_constraint(x, pltpu.HBM) for x in operands]
        outs += [jax.ShapeDtypeStruct((2, 1, units), F32)] * 2 + [jax.ShapeDtypeStruct((1, features), F32)]
    outs = pl.pallas_call(
        fetching_kernel if small else products_kernel,
        out_shape=outs,
        in_specs=[HBM if small else VMEM] * len(operands),
        out_specs=[VMEM] * len(outs),
        scratch_shapes=scratch if small else scratch[:1],
        compiler_params=PARAMS,
        cost_estimate=pl.CostEstimate(
            flops=4 * tokens * features * units, bytes_accessed=8 * features * units, transcendentals=0
        ),
    )(*operands)
    return outs[:SIDE], outs[SIDE:]


def total_of(refs):
    return sum(ref[...].astype(F32) for ref in refs[1:]) + refs[0][...].astype(F32)


def add_kernel(*refs):
    *in_refs, out_ref = refs
    end = out_ref.shape[0] - 8
    total = total_of(in_refs)
    out_ref[:end] = total[:end].astype(BF16)
    squares = whole_squares(total[end:])
    high = squares.astype(BF16).astype(F32)
    lane = lax.broadcasted_iota(jnp.int32, squares.shape, 1)
    out_ref[end:] = jnp.where(lane % 2 == 0, high, pltpu.roll(squares - high, 1, 1)).astype(BF16)


def hidden_kernel(*refs):
    *in_refs, scales_ref, out_ref = refs
    rows, units = out_ref.shape
    total = total_of(in_refs)
    inverse = lax.rsqrt(whole_squares(total[2 * units // 128 * rows :]) / D + 1e-06)
    inverse = jnp.concatenate([inverse[:, 2 * k : 2 * k + 1] for k in range(rows // 8)])
    for n in range(units // 128):
        columns = slice(n * 128, (n + 1) * 128)
        gate = inverse * scales_ref[0, :, columns] * total[n * rows : (n + 1) * rows]
        m = n + units // 128
        up = inverse * scales_ref[1, :, columns] * total[m * rows : (m + 1) * rows]
        out_ref[:, columns] = (gate / (1.0 + jnp.exp(-gate)) * up).astype(BF16)


def down_kernel(*refs):
    *in_refs, w_ref, out_ref, hidden = refs
    rows = in_refs[0].shape[0]
    place = place_in_f()
    for k, ref in enumerate(in_refs):
        at = pl.multiple_of((place ^ k) * rows, rows)
        hidden[pl.ds(at, rows)] = ref[...]
    out_ref[...] = lax.dot_general(
        w_ref[...].astype(BF16), hidden[...], (((1,), (1,)), ((), ())), preferred_element_type=F32
    ).astype(BF16)


def call(kernel, shape, *operands, scratch=(), flops=0):
    return pl.pallas_call(
        kernel,
        out_shape=jax.ShapeDtypeStruct(shape, BF16),
        in_specs=[VMEM] * len(operands),
        out_specs=VMEM,
        scratch_shapes=scratch,
        compiler_params=PARAMS,
        cost_estimate=pl.CostEstimate(
            flops=flops or 8 * operands[0].size,
            bytes_accessed=sum(x.size * x.dtype.itemsize for x in operands),
            transcendentals=0,
        ),
    )(*operands)


def half_step(stream, blocks, scales, w_down, down_scale):
    rows, units = stream.shape[1] // SIDE, scales.shape[2]
    mine = call(add_kernel, blocks[0].shape, blocks[0], *(swapped(blocks[k], k, True) for k in ORDER))
    peers = [swapped(mine, k, False) for k in ORDER]
    hidden = call(hidden_kernel, (rows, units), mine, *peers, scales)
    others = {k: swapped(hidden, k, True) for k in ORDER}
    features = w_down.shape[1]
    tokens = stream.shape[1]
    down = call(
        down_kernel,
        (features, tokens),
        hidden,
        others[1],
        others[2],
        others[3],
        w_down.T,
        scratch=[pltpu.VMEM((tokens, units), BF16)],
        flops=2 * tokens * units * features,
    )
    return (stream.astype(F32) + 0.5 * down_scale[:, None] * sum_over_cb(down)).astype(BF16)


def body(
    tokens,
    first_gain,
    first_gate,
    first_up,
    first_down,
    first_gate_scale,
    first_up_scale,
    first_down_scale,
    second_gain,
    second_gate,
    second_up,
    second_down,
    second_gate_scale,
    second_up_scale,
    second_down_scale,
):
    stream = tokens.T
    small = (first_gate_scale, first_up_scale, second_gate_scale, second_up_scale, second_gain)
    blocks, (scales, later_scales, later_gain) = products(
        stream, first_gain[None, :], first_gate, first_up, *(x[None, :] for x in small)
    )
    middle = half_step(stream, blocks, scales, first_down, first_down_scale)
    blocks, _ = products(middle, later_gain, second_gate, second_up)
    return half_step(middle, blocks, later_scales, second_down, second_down_scale).T


def solution(mesh):
    one = (P("ra"), P("ra", "cb"), P("ra", "cb"), P("cb", "ra"), P("cb"), P("cb"), P("ra"))
    return jax.shard_map(
        body, mesh=mesh, in_specs=(P(None, "ra"), *one, *one), out_specs=P(None, "ra"), check_vma=False
    )
```

```python
import functools

import jax
import jax.numpy as jnp
from jax import lax
from jax.experimental import pallas as pl
from jax.experimental.pallas import tpu as pltpu
from jax.sharding import PartitionSpec as P


D = 3072
SIDE = 4
WIDE = 1024
PIECE = 96
ORDER = (2, 1, 3)
X_ORDER = (2, 1, 3)
BF16 = jnp.bfloat16
F32 = jnp.float32
VMEM = pl.BlockSpec(memory_space=pltpu.VMEM)
HBM = pl.BlockSpec(memory_space=pltpu.HBM)
PARAMS = pltpu.CompilerParams(vmem_limit_bytes=12 << 20)


def rounded(x):
    return lax.reduce_precision(x, 8, 7)


def place_in_f():
    ra, cb = lax.axis_index("ra"), lax.axis_index("cb")
    return jnp.where(cb % 2 == 0, ra // SIDE, ra % SIDE)


def pairs_of(k, along_f):
    pairs = []
    for z in range(SIDE):
        for y in range(SIDE):
            for cb in range(8):
                if (cb % 2 == 0) == along_f:
                    to = (z ^ k, y)
                else:
                    to = (z, y ^ k)
                pairs.append(((z * SIDE + y) * 8 + cb, (to[0] * SIDE + to[1]) * 8 + cb))
    return pairs


def swapped(x, k, along_f):
    return lax.ppermute(x, ("ra", "cb"), pairs_of(k, along_f))


def other_core(x):
    return lax.ppermute(x, "cb", [(i, i ^ 1) for i in range(lax.axis_size("cb"))])


def sum_over_x(chip):
    sent = chip.astype(BF16)
    n = lax.axis_size("cb")
    others = {k: lax.ppermute(sent, "cb", [(i, i ^ 2 * k) for i in range(n)]).astype(F32) for k in X_ORDER}
    return (chip + others[2]) + (others[1] + others[3])


def packed_squares(squares):
    high = squares.astype(BF16).astype(F32)
    low = squares - high
    lane = lax.broadcasted_iota(jnp.int32, (8, 128), 1)
    tile = jnp.zeros((8, 128), F32)
    for k in range(squares.shape[0] // 8):
        tile = jnp.where(lane == 2 * k, high[8 * k : 8 * k + 8], tile)
        tile = jnp.where(lane == 2 * k + 1, low[8 * k : 8 * k + 8], tile)
    return tile.astype(BF16)


def whole_squares(tile):
    return tile + pltpu.roll(tile, 127, 1)


def turned_rows(stream_ref, turned):
    tokens = stream_ref.shape[1]
    rows = tokens // SIDE
    turned[0] = stream_ref[...].astype(F32).T
    place = place_in_f()
    for k in range(SIDE):
        at = pl.multiple_of((place ^ k) * rows, rows)
        turned[1, k * rows : (k + 1) * rows] = turned[0, pl.ds(at, rows)]
    return turned[1]


def write_products(stream, gain, pieces, out_refs):
    rows = stream.shape[0] // SIDE
    squares = jnp.sum(stream * stream, axis=1, keepdims=True)
    for k, out_ref in enumerate(out_refs):
        out_ref[len(pieces) * WIDE // 128 * rows :] = packed_squares(squares[k * rows : (k + 1) * rows])
    shaped = (stream * gain).astype(BF16)
    for c, piece in enumerate(pieces):
        part = jnp.dot(shaped, piece().astype(BF16), preferred_element_type=F32).astype(BF16)
        for k, out_ref in enumerate(out_refs):
            for n in range(WIDE // 128):
                at = (c * WIDE // 128 + n) * rows
                out_ref[at : at + rows] = part[k * rows : (k + 1) * rows, n * 128 : (n + 1) * 128]


def fetching_kernel(stream_ref, gain_ref, gate_ref, up_ref, *refs):
    small_refs, refs = refs[:5], refs[5:]
    out_refs, refs = refs[:SIDE], refs[SIDE:]
    half_ref, scales_ref, later_scales_ref, later_gain_ref, turned, stream_held, gain_held, held, sems, small_sems = refs
    targets = (
        stream_held,
        gain_held,
        scales_ref.at[0],
        scales_ref.at[1],
        later_scales_ref.at[0],
        later_scales_ref.at[1],
        later_gain_ref,
    )
    small = [
        pltpu.make_async_copy(ref, target, small_sems.at[k])
        for k, (ref, target) in enumerate(zip((stream_ref, gain_ref, *small_refs), targets, strict=True))
    ]
    for copy in small[:2]:
        copy.start()
    copies = [
        pltpu.make_async_copy(ref.at[pl.ds(at, PIECE)], held.at[n, pl.ds(at, PIECE)], sems.at[n, at // PIECE])
        for n, ref in enumerate((gate_ref, up_ref))
        for at in range(0, ref.shape[0], PIECE)
    ]
    for copy in copies:
        copy.start()
    for copy in small[2:]:
        copy.start()

    def piece(n, at):
        if at == 0:
            for copy in copies[n * len(copies) // 2 : (n + 1) * len(copies) // 2]:
                copy.wait()
        return held[n, :, at : at + WIDE]

    small[0].wait()
    stream = turned_rows(stream_held, turned)
    near = pl.multiple_of(lax.axis_index("cb") % 2 * half_ref.shape[1], half_ref.shape[1])
    half_ref[...] = stream_held[:, pl.ds(near, half_ref.shape[1])]
    small[1].wait()
    pieces = [functools.partial(piece, n, at) for n in range(2) for at in range(0, held.shape[2], WIDE)]
    write_products(stream, gain_held[...], pieces, out_refs)
    for copy in small[2:]:
        copy.wait()


def products_kernel(stream_ref, gain_ref, *refs):
    w_refs, (*out_refs, turned) = refs[: -SIDE - 1], refs[-SIDE - 1 :]

    def piece(ref, at):
        return ref[:, at : at + WIDE]

    pieces = [functools.partial(piece, ref, at) for ref in w_refs for at in range(0, ref.shape[1], WIDE)]
    write_products(turned_rows(stream_ref, turned), gain_ref[...], pieces, out_refs)


def products(stream, gain, weights, small=()):
    features, tokens = stream.shape
    columns = sum(w.shape[1] for w in weights)
    units = weights[0].shape[1]
    scratch = [
        pltpu.VMEM((2, tokens, features), F32),
        pltpu.VMEM((features, tokens), BF16),
        pltpu.VMEM((1, features), F32),
        pltpu.VMEM((2, features, units), F32),
        pltpu.SemaphoreType.DMA((2, features // PIECE)),
        pltpu.SemaphoreType.DMA((7,)),
    ]
    operands = [stream, gain, *weights, *small]
    rows = tokens // SIDE
    outs = [jax.ShapeDtypeStruct((columns // 128 * rows + 8, 128), BF16)] * SIDE
    if small:
        operands = [pltpu.with_memory_space_constraint(x, pltpu.HBM) for x in operands]
        outs += [jax.ShapeDtypeStruct((features, tokens // 2), BF16)]
        outs += [jax.ShapeDtypeStruct((2, 1, units), F32)] * 2 + [jax.ShapeDtypeStruct((1, features), F32)]
    outs = pl.pallas_call(
        fetching_kernel if small else products_kernel,
        out_shape=outs,
        in_specs=[HBM if small else VMEM] * len(operands),
        out_specs=[VMEM] * len(outs),
        scratch_shapes=scratch if small else scratch[:1],
        compiler_params=PARAMS,
        cost_estimate=pl.CostEstimate(
            flops=2 * tokens * features * columns, bytes_accessed=4 * features * columns, transcendentals=0
        ),
    )(*operands)
    return outs[:SIDE], outs[SIDE:]


def total_of(refs):
    return sum(ref[...].astype(F32) for ref in refs[1:]) + refs[0][...].astype(F32)


def add_kernel(*refs):
    *in_refs, out_ref = refs
    end = out_ref.shape[0] - 8
    total = total_of(in_refs)
    out_ref[:end] = total[:end].astype(BF16)
    squares = whole_squares(total[end:])
    high = squares.astype(BF16).astype(F32)
    lane = lax.broadcasted_iota(jnp.int32, squares.shape, 1)
    out_ref[end:] = jnp.where(lane % 2 == 0, high, pltpu.roll(squares - high, 1, 1)).astype(BF16)


def hidden_kernel(count, *refs):
    in_refs, scales_refs, out_ref = refs[:SIDE], refs[SIDE : SIDE + count], refs[-1]
    rows, units = out_ref.shape
    each = units // count
    total = total_of(in_refs)
    inverse = lax.rsqrt(whole_squares(total[2 * units // 128 * rows :]) / D + 1e-06)
    inverse = jnp.concatenate([inverse[:, 2 * k : 2 * k + 1] for k in range(rows // 8)])
    for n in range(units // 128):
        scales_ref, at = scales_refs[n * 128 // each], n * 128 % each
        gate = inverse * scales_ref[0, :, at : at + 128] * total[n * rows : (n + 1) * rows]
        m = n + units // 128
        up = inverse * scales_ref[1, :, at : at + 128] * total[m * rows : (m + 1) * rows]
        out_ref[:, n * 128 : (n + 1) * 128] = (gate / (1.0 + jnp.exp(-gate)) * up).astype(BF16)


def down_kernel(count, *refs):
    in_refs, w_refs, (*out_refs, hidden) = refs[:SIDE], refs[SIDE : SIDE + count], refs[SIDE + count :]
    rows = in_refs[0].shape[0]
    tokens = rows * SIDE
    place = place_in_f()
    turn = lax.axis_index("cb") % 2 * (SIDE // 2) if len(out_refs) == 2 else 0
    for k, ref in enumerate(in_refs):
        at = pl.multiple_of(((place ^ k) + turn) % SIDE * rows, rows)
        hidden[pl.ds(at, rows)] = ref[...]
    each = hidden.shape[1] // count
    for n, out_ref in enumerate(out_refs):
        wide = tokens // len(out_refs)
        parts = [
            lax.dot_general(
                w_ref[...].astype(BF16),
                hidden[n * wide : (n + 1) * wide, k * each : (k + 1) * each],
                (((1,), (1,)), ((), ())),
                preferred_element_type=F32,
            )
            for k, w_ref in enumerate(w_refs)
        ]
        out_ref[...] = functools.reduce(jnp.add, parts).astype(BF16)


def call(kernel, shapes, *operands, scratch=(), flops=0):
    return pl.pallas_call(
        kernel,
        out_shape=[jax.ShapeDtypeStruct(shape, BF16) for shape in shapes],
        in_specs=[VMEM] * len(operands),
        out_specs=[VMEM] * len(shapes),
        scratch_shapes=scratch,
        compiler_params=PARAMS,
        cost_estimate=pl.CostEstimate(
            flops=flops or 8 * operands[0].size,
            bytes_accessed=sum(x.size * x.dtype.itemsize for x in operands),
            transcendentals=0,
        ),
    )(*operands)


def hidden_blocks(mine, scales):
    peers = [swapped(mine, k, False) for k in ORDER]
    units = sum(x.shape[2] for x in scales)
    rows = mine.shape[0] // (2 * units // 128)
    kernel = functools.partial(hidden_kernel, len(scales))
    (hidden,) = call(kernel, [(rows, units)], mine, *peers, *scales)
    others = {k: swapped(hidden, k, True) for k in ORDER}
    return hidden, others[1], others[2], others[3]


def down_products(blocks, weights, outs):
    rows, units = blocks[0].shape
    tokens, features = rows * SIDE, weights[0].shape[1]
    return call(
        functools.partial(down_kernel, len(weights)),
        [(features, tokens // outs)] * outs,
        *blocks,
        *(w.T for w in weights),
        scratch=[pltpu.VMEM((tokens, units), BF16)],
        flops=2 * tokens * units * features,
    )


def step_result(stream, down_scale, down):
    return (stream.astype(F32) + 0.5 * down_scale[:, None] * down).astype(BF16)


def body(
    tokens,
    first_gain,
    first_gate,
    first_up,
    first_down,
    first_gate_scale,
    first_up_scale,
    first_down_scale,
    second_gain,
    second_gate,
    second_up,
    second_down,
    second_gate_scale,
    second_up_scale,
    second_down_scale,
):
    small = (first_gate_scale, first_up_scale, second_gate_scale, second_up_scale, second_gain)
    blocks, (half, scales, later_scales, later_gain) = products(
        tokens.T, first_gain[None, :], (first_gate, first_up), [x[None, :] for x in small]
    )
    received = [swapped(blocks[k], k, True) for k in ORDER]
    theirs = [other_core(x) for x in (second_gate, second_up, second_down.T, later_scales)]
    received, theirs = lax.optimization_barrier((received, theirs))
    their_gate, their_up, their_down, their_scales = theirs
    (mine,) = call(add_kernel, [blocks[0].shape], blocks[0], *received)
    near, far = down_products(hidden_blocks(mine, [scales]), [first_down], 2)
    chip = rounded(near.astype(F32) + other_core(far).astype(F32))
    middle = step_result(half, first_down_scale, sum_over_x(chip))

    blocks, _ = products(middle, later_gain, (second_gate, their_gate, second_up, their_up))
    received = [swapped(blocks[k], k, True) for k in ORDER]
    (mine,) = call(add_kernel, [blocks[0].shape], blocks[0], *received)
    hidden = hidden_blocks(mine, [later_scales, their_scales])
    (down,) = down_products(hidden, [second_down, their_down.T], 1)
    mixed = step_result(middle, second_down_scale, sum_over_x(down.astype(F32)))
    other = other_core(mixed)
    first = lax.axis_index("cb") % 2 == 0
    both = jnp.where(first, jnp.concatenate([mixed, other], axis=1), jnp.concatenate([other, mixed], axis=1))
    return both.T


def solution(mesh):
    one = (P("ra"), P("ra", "cb"), P("ra", "cb"), P("cb", "ra"), P("cb"), P("cb"), P("ra"))
    return jax.shard_map(
        body, mesh=mesh, in_specs=(P(None, "ra"), *one, *one), out_specs=P(None, "ra"), check_vma=False
    )
```

```python
import functools

import jax
import jax.numpy as jnp
from jax import lax
from jax.experimental import pallas as pl
from jax.experimental.pallas import tpu as pltpu
from jax.sharding import PartitionSpec as P


D = 3072
SIDE = 4
WIDE = 1024
PIECE = 96
ORDER = (2, 3, 1)
X_ORDER = (2, 3, 1)
G_ORDER = (2, 3, 1)
BF16 = jnp.bfloat16
F32 = jnp.float32
VMEM = pl.BlockSpec(memory_space=pltpu.VMEM)
HBM = pl.BlockSpec(memory_space=pltpu.HBM)
PARAMS = pltpu.CompilerParams(vmem_limit_bytes=12 << 20)


def rounded(x):
    return lax.reduce_precision(x, 8, 7)


def place_in_f():
    ra, cb = lax.axis_index("ra"), lax.axis_index("cb")
    return jnp.where(cb % 2 == 0, ra // SIDE, ra % SIDE)


def pairs_of(k, along_f):
    pairs = []
    for z in range(SIDE):
        for y in range(SIDE):
            for cb in range(8):
                if (cb % 2 == 0) == along_f:
                    to = (z ^ k, y)
                else:
                    to = (z, y ^ k)
                pairs.append(((z * SIDE + y) * 8 + cb, (to[0] * SIDE + to[1]) * 8 + cb))
    return pairs


def swapped(x, k, along_f):
    return lax.ppermute(x, ("ra", "cb"), pairs_of(k, along_f))


def other_core(x):
    return lax.ppermute(x, "cb", [(i, i ^ 1) for i in range(lax.axis_size("cb"))])


def sum_over_x(chip):
    sent = chip.astype(BF16)
    n = lax.axis_size("cb")
    others = {k: lax.ppermute(sent, "cb", [(i, i ^ 2 * k) for i in range(n)]).astype(F32) for k in X_ORDER}
    return (chip + others[2]) + (others[1] + others[3])


def packed_squares(squares):
    high = squares.astype(BF16).astype(F32)
    low = squares - high
    lane = lax.broadcasted_iota(jnp.int32, (8, 128), 1)
    tile = jnp.zeros((8, 128), F32)
    for k in range(squares.shape[0] // 8):
        tile = jnp.where(lane == 2 * k, high[8 * k : 8 * k + 8], tile)
        tile = jnp.where(lane == 2 * k + 1, low[8 * k : 8 * k + 8], tile)
    return tile.astype(BF16)


def whole_squares(tile):
    return tile + pltpu.roll(tile, 127, 1)


def turned_rows(stream_ref, turned):
    tokens = stream_ref.shape[1]
    rows = tokens // SIDE
    turned[0] = stream_ref[...].astype(F32).T
    place = place_in_f()
    for k in range(SIDE):
        at = pl.multiple_of((place ^ k) * rows, rows)
        turned[1, k * rows : (k + 1) * rows] = turned[0, pl.ds(at, rows)]
    return turned[1]


def write_products(stream, gain, pieces, out_refs):
    rows = stream.shape[0] // SIDE
    squares = jnp.sum(stream * stream, axis=1, keepdims=True)
    for k, out_ref in enumerate(out_refs):
        out_ref[len(pieces) * WIDE // 128 * rows :] = packed_squares(squares[k * rows : (k + 1) * rows])
    shaped = (stream * gain).astype(BF16)
    for c, piece in enumerate(pieces):
        part = jnp.dot(shaped, piece().astype(BF16), preferred_element_type=F32).astype(BF16)
        for k, out_ref in enumerate(out_refs):
            for n in range(WIDE // 128):
                at = (c * WIDE // 128 + n) * rows
                out_ref[at : at + rows] = part[k * rows : (k + 1) * rows, n * 128 : (n + 1) * 128]


def fetching_kernel(stream_ref, gain_ref, gate_ref, up_ref, *refs):
    small_refs, refs = refs[:5], refs[5:]
    out_refs, refs = refs[:SIDE], refs[SIDE:]
    half_ref, scales_ref, later_scales_ref, later_gain_ref, turned, stream_held, gain_held, held, sems, small_sems = refs
    targets = (
        stream_held,
        gain_held,
        scales_ref.at[0],
        scales_ref.at[1],
        later_scales_ref.at[0],
        later_scales_ref.at[1],
        later_gain_ref,
    )
    small = [
        pltpu.make_async_copy(ref, target, small_sems.at[k])
        for k, (ref, target) in enumerate(zip((stream_ref, gain_ref, *small_refs), targets, strict=True))
    ]
    for copy in small[:2]:
        copy.start()
    copies = [
        pltpu.make_async_copy(ref.at[pl.ds(at, PIECE)], held.at[n, pl.ds(at, PIECE)], sems.at[n, at // PIECE])
        for n, ref in enumerate((gate_ref, up_ref))
        for at in range(0, ref.shape[0], PIECE)
    ]
    for copy in copies:
        copy.start()
    for copy in small[2:]:
        copy.start()

    def piece(n, at):
        if at == 0:
            for copy in copies[n * len(copies) // 2 : (n + 1) * len(copies) // 2]:
                copy.wait()
        return held[n, :, at : at + WIDE]

    small[0].wait()
    stream = turned_rows(stream_held, turned)
    near = pl.multiple_of(lax.axis_index("cb") % 2 * half_ref.shape[1], half_ref.shape[1])
    half_ref[...] = stream_held[:, pl.ds(near, half_ref.shape[1])]
    small[1].wait()
    pieces = [functools.partial(piece, n, at) for n in range(2) for at in range(0, held.shape[2], WIDE)]
    write_products(stream, gain_held[...], pieces, out_refs)
    for copy in small[2:]:
        copy.wait()


def products_kernel(stream_ref, gain_ref, *refs):
    w_refs, (*out_refs, turned) = refs[: -SIDE - 1], refs[-SIDE - 1 :]

    def piece(ref, at):
        return ref[:, at : at + WIDE]

    pieces = [functools.partial(piece, ref, at) for ref in w_refs for at in range(0, ref.shape[1], WIDE)]
    write_products(turned_rows(stream_ref, turned), gain_ref[...], pieces, out_refs)


def products(stream, gain, weights, small=()):
    features, tokens = stream.shape
    columns = sum(w.shape[1] for w in weights)
    units = weights[0].shape[1]
    scratch = [
        pltpu.VMEM((2, tokens, features), F32),
        pltpu.VMEM((features, tokens), BF16),
        pltpu.VMEM((1, features), F32),
        pltpu.VMEM((2, features, units), F32),
        pltpu.SemaphoreType.DMA((2, features // PIECE)),
        pltpu.SemaphoreType.DMA((7,)),
    ]
    operands = [stream, gain, *weights, *small]
    rows = tokens // SIDE
    outs = [jax.ShapeDtypeStruct((columns // 128 * rows + 8, 128), BF16)] * SIDE
    if small:
        operands = [pltpu.with_memory_space_constraint(x, pltpu.HBM) for x in operands]
        outs += [jax.ShapeDtypeStruct((features, tokens // 2), BF16)]
        outs += [jax.ShapeDtypeStruct((2, 1, units), F32)] * 2 + [jax.ShapeDtypeStruct((1, features), F32)]
    outs = pl.pallas_call(
        fetching_kernel if small else products_kernel,
        out_shape=outs,
        in_specs=[HBM if small else VMEM] * len(operands),
        out_specs=[VMEM] * len(outs),
        scratch_shapes=scratch if small else scratch[:1],
        compiler_params=PARAMS,
        cost_estimate=pl.CostEstimate(
            flops=2 * tokens * features * columns, bytes_accessed=4 * features * columns, transcendentals=0
        ),
    )(*operands)
    return outs[:SIDE], outs[SIDE:]


def total_of(refs):
    return sum(ref[...].astype(F32) for ref in refs[1:]) + refs[0][...].astype(F32)


def add_kernel(*refs):
    *in_refs, out_ref = refs
    end = out_ref.shape[0] - 8
    total = total_of(in_refs)
    out_ref[:end] = total[:end].astype(BF16)
    squares = whole_squares(total[end:])
    high = squares.astype(BF16).astype(F32)
    lane = lax.broadcasted_iota(jnp.int32, squares.shape, 1)
    out_ref[end:] = jnp.where(lane % 2 == 0, high, pltpu.roll(squares - high, 1, 1)).astype(BF16)


def hidden_kernel(count, *refs):
    in_refs, scales_refs, out_ref = refs[:SIDE], refs[SIDE : SIDE + count], refs[-1]
    rows, units = out_ref.shape
    each = units // count
    total = total_of(in_refs)
    inverse = lax.rsqrt(whole_squares(total[2 * units // 128 * rows :]) / D + 1e-06)
    inverse = jnp.concatenate([inverse[:, 2 * k : 2 * k + 1] for k in range(rows // 8)])
    for n in range(units // 128):
        scales_ref, at = scales_refs[n * 128 // each], n * 128 % each
        gate = inverse * scales_ref[0, :, at : at + 128] * total[n * rows : (n + 1) * rows]
        m = n + units // 128
        up = inverse * scales_ref[1, :, at : at + 128] * total[m * rows : (m + 1) * rows]
        out_ref[:, n * 128 : (n + 1) * 128] = (gate / (1.0 + jnp.exp(-gate)) * up).astype(BF16)


def down_kernel(count, *refs):
    in_refs, w_refs, (*out_refs, hidden) = refs[:SIDE], refs[SIDE : SIDE + count], refs[SIDE + count :]
    rows = in_refs[0].shape[0]
    tokens = rows * SIDE
    place = place_in_f()
    turn = lax.axis_index("cb") % 2 * (SIDE // 2) if len(out_refs) == 2 else 0
    for k, ref in enumerate(in_refs):
        at = pl.multiple_of(((place ^ k) + turn) % SIDE * rows, rows)
        hidden[pl.ds(at, rows)] = ref[...]
    each = hidden.shape[1] // count
    for n, out_ref in enumerate(out_refs):
        wide = tokens // len(out_refs)
        parts = [
            lax.dot_general(
                w_ref[...].astype(BF16),
                hidden[n * wide : (n + 1) * wide, k * each : (k + 1) * each],
                (((1,), (1,)), ((), ())),
                preferred_element_type=F32,
            )
            for k, w_ref in enumerate(w_refs)
        ]
        out_ref[...] = functools.reduce(jnp.add, parts).astype(BF16)


def call(kernel, shapes, *operands, scratch=(), flops=0):
    return pl.pallas_call(
        kernel,
        out_shape=[jax.ShapeDtypeStruct(shape, BF16) for shape in shapes],
        in_specs=[VMEM] * len(operands),
        out_specs=[VMEM] * len(shapes),
        scratch_shapes=scratch,
        compiler_params=PARAMS,
        cost_estimate=pl.CostEstimate(
            flops=flops or 8 * operands[0].size,
            bytes_accessed=sum(x.size * x.dtype.itemsize for x in operands),
            transcendentals=0,
        ),
    )(*operands)


def hidden_blocks(mine, scales):
    peers = [swapped(mine, k, False) for k in ORDER]
    units = sum(x.shape[2] for x in scales)
    rows = mine.shape[0] // (2 * units // 128)
    kernel = functools.partial(hidden_kernel, len(scales))
    (hidden,) = call(kernel, [(rows, units)], mine, *peers, *scales)
    others = {k: swapped(hidden, k, True) for k in G_ORDER}
    return hidden, others[1], others[2], others[3]


def down_products(blocks, weights, outs):
    rows, units = blocks[0].shape
    tokens, features = rows * SIDE, weights[0].shape[1]
    return call(
        functools.partial(down_kernel, len(weights)),
        [(features, tokens // outs)] * outs,
        *blocks,
        *(w.T for w in weights),
        scratch=[pltpu.VMEM((tokens, units), BF16)],
        flops=2 * tokens * units * features,
    )


def step_result(stream, down_scale, down):
    return (stream.astype(F32) + 0.5 * down_scale[:, None] * down).astype(BF16)


def body(
    tokens,
    first_gain,
    first_gate,
    first_up,
    first_down,
    first_gate_scale,
    first_up_scale,
    first_down_scale,
    second_gain,
    second_gate,
    second_up,
    second_down,
    second_gate_scale,
    second_up_scale,
    second_down_scale,
):
    small = (first_gate_scale, first_up_scale, second_gate_scale, second_up_scale, second_gain)
    blocks, (half, scales, later_scales, later_gain) = products(
        tokens.T, first_gain[None, :], (first_gate, first_up), [x[None, :] for x in small]
    )
    received = [swapped(blocks[k], k, True) for k in ORDER]
    theirs = [other_core(x) for x in (second_gate, second_up, second_down.T, later_scales)]
    received, theirs = lax.optimization_barrier((received, theirs))
    their_gate, their_up, their_down, their_scales = theirs
    (mine,) = call(add_kernel, [blocks[0].shape], blocks[0], *received)
    near, far = down_products(hidden_blocks(mine, [scales]), [first_down], 2)
    chip = rounded(near.astype(F32) + other_core(far).astype(F32))
    middle = step_result(half, first_down_scale, sum_over_x(chip))

    blocks, _ = products(middle, later_gain, (second_gate, their_gate, second_up, their_up))
    received = [swapped(blocks[k], k, True) for k in ORDER]
    (mine,) = call(add_kernel, [blocks[0].shape], blocks[0], *received)
    hidden = hidden_blocks(mine, [later_scales, their_scales])
    (down,) = down_products(hidden, [second_down, their_down.T], 1)
    mixed = step_result(middle, second_down_scale, sum_over_x(down.astype(F32)))
    other = other_core(mixed)
    first = lax.axis_index("cb") % 2 == 0
    both = jnp.where(first, jnp.concatenate([mixed, other], axis=1), jnp.concatenate([other, mixed], axis=1))
    return both.T


def solution(mesh):
    one = (P("ra"), P("ra", "cb"), P("ra", "cb"), P("cb", "ra"), P("cb"), P("cb"), P("ra"))
    return jax.shard_map(
        body, mesh=mesh, in_specs=(P(None, "ra"), *one, *one), out_specs=P(None, "ra"), check_vma=False
    )
```

```python
import functools

import jax
import jax.numpy as jnp
from jax import lax
from jax.experimental import pallas as pl
from jax.experimental.pallas import tpu as pltpu
from jax.sharding import PartitionSpec as P


D = 3072
SIDE = 4
WIDE = 512
PIECE = 96
ORDER = (2, 3, 1)
X_ORDER = (2, 3, 1)
G_ORDER = (2, 3, 1)
BF16 = jnp.bfloat16
F32 = jnp.float32
VMEM = pl.BlockSpec(memory_space=pltpu.VMEM)
HBM = pl.BlockSpec(memory_space=pltpu.HBM)
PARAMS = pltpu.CompilerParams(vmem_limit_bytes=12 << 20)


def rounded(x):
    return lax.reduce_precision(x, 8, 7)


def place_in_f():
    ra, cb = lax.axis_index("ra"), lax.axis_index("cb")
    return jnp.where(cb % 2 == 0, ra // SIDE, ra % SIDE)


def pairs_of(k, along_f):
    pairs = []
    for z in range(SIDE):
        for y in range(SIDE):
            for cb in range(8):
                if (cb % 2 == 0) == along_f:
                    to = (z ^ k, y)
                else:
                    to = (z, y ^ k)
                pairs.append(((z * SIDE + y) * 8 + cb, (to[0] * SIDE + to[1]) * 8 + cb))
    return pairs


def swapped(x, k, along_f):
    return lax.ppermute(x, ("ra", "cb"), pairs_of(k, along_f))


def other_core(x):
    return lax.ppermute(x, "cb", [(i, i ^ 1) for i in range(lax.axis_size("cb"))])


def sum_over_x(chip):
    sent = chip.astype(BF16)
    n = lax.axis_size("cb")
    others = {k: lax.ppermute(sent, "cb", [(i, i ^ 2 * k) for i in range(n)]).astype(F32) for k in X_ORDER}
    return (chip + others[2]) + (others[1] + others[3])


def packed_squares(squares):
    high = squares.astype(BF16).astype(F32)
    low = squares - high
    lane = lax.broadcasted_iota(jnp.int32, (8, 128), 1)
    tile = jnp.zeros((8, 128), F32)
    for k in range(squares.shape[0] // 8):
        tile = jnp.where(lane == 2 * k, high[8 * k : 8 * k + 8], tile)
        tile = jnp.where(lane == 2 * k + 1, low[8 * k : 8 * k + 8], tile)
    return tile.astype(BF16)


def whole_squares(tile):
    return tile + pltpu.roll(tile, 127, 1)


def turned_rows(stream_ref, turned):
    tokens = stream_ref.shape[1]
    rows = tokens // SIDE
    turned[0] = stream_ref[...].astype(F32).T
    place = place_in_f()
    for k in range(SIDE):
        at = pl.multiple_of((place ^ k) * rows, rows)
        turned[1, k * rows : (k + 1) * rows] = turned[0, pl.ds(at, rows)]
    return turned[1]


def write_products(stream, gain, pieces, out_refs):
    rows = stream.shape[0] // SIDE
    squares = jnp.sum(stream * stream, axis=1, keepdims=True)
    for k, out_ref in enumerate(out_refs):
        out_ref[len(pieces) * WIDE // 128 * rows :] = packed_squares(squares[k * rows : (k + 1) * rows])
    shaped = (stream * gain).astype(BF16)
    for c, piece in enumerate(pieces):
        part = jnp.dot(shaped, piece().astype(BF16), preferred_element_type=F32).astype(BF16)
        for k, out_ref in enumerate(out_refs):
            for n in range(WIDE // 128):
                at = (c * WIDE // 128 + n) * rows
                out_ref[at : at + rows] = part[k * rows : (k + 1) * rows, n * 128 : (n + 1) * 128]


def fetching_kernel(stream_ref, gain_ref, gate_ref, up_ref, *refs):
    small_refs, refs = refs[:5], refs[5:]
    out_refs, refs = refs[:SIDE], refs[SIDE:]
    half_ref, scales_ref, later_scales_ref, later_gain_ref, turned, stream_held, gain_held, held, sems, small_sems = refs
    targets = (
        stream_held,
        gain_held,
        scales_ref.at[0],
        scales_ref.at[1],
        later_scales_ref.at[0],
        later_scales_ref.at[1],
        later_gain_ref,
    )
    small = [
        pltpu.make_async_copy(ref, target, small_sems.at[k])
        for k, (ref, target) in enumerate(zip((stream_ref, gain_ref, *small_refs), targets, strict=True))
    ]
    for copy in small:
        copy.start()
    copies = [
        pltpu.make_async_copy(ref.at[pl.ds(at, PIECE)], held.at[n, pl.ds(at, PIECE)], sems.at[n, at // PIECE])
        for n, ref in enumerate((gate_ref, up_ref))
        for at in range(0, ref.shape[0], PIECE)
    ]
    for copy in copies:
        copy.start()

    def piece(n, at):
        if at == 0:
            for copy in copies[n * len(copies) // 2 : (n + 1) * len(copies) // 2]:
                copy.wait()
        return held[n, :, at : at + WIDE]

    small[0].wait()
    stream = turned_rows(stream_held, turned)
    near = pl.multiple_of(lax.axis_index("cb") % 2 * half_ref.shape[1], half_ref.shape[1])
    half_ref[...] = stream_held[:, pl.ds(near, half_ref.shape[1])]
    small[1].wait()
    pieces = [functools.partial(piece, n, at) for n in range(2) for at in range(0, held.shape[2], WIDE)]
    write_products(stream, gain_held[...], pieces, out_refs)
    for copy in small[2:]:
        copy.wait()


def products_kernel(stream_ref, gain_ref, *refs):
    w_refs, (*out_refs, turned) = refs[: -SIDE - 1], refs[-SIDE - 1 :]

    def piece(ref, at):
        return ref[:, at : at + WIDE]

    pieces = [functools.partial(piece, ref, at) for ref in w_refs for at in range(0, ref.shape[1], WIDE)]
    write_products(turned_rows(stream_ref, turned), gain_ref[...], pieces, out_refs)


def products(stream, gain, weights, small=()):
    features, tokens = stream.shape
    columns = sum(w.shape[1] for w in weights)
    units = weights[0].shape[1]
    scratch = [
        pltpu.VMEM((2, tokens, features), F32),
        pltpu.VMEM((features, tokens), BF16),
        pltpu.VMEM((1, features), F32),
        pltpu.VMEM((2, features, units), F32),
        pltpu.SemaphoreType.DMA((2, features // PIECE)),
        pltpu.SemaphoreType.DMA((7,)),
    ]
    operands = [stream, gain, *weights, *small]
    rows = tokens // SIDE
    outs = [jax.ShapeDtypeStruct((columns // 128 * rows + 8, 128), BF16)] * SIDE
    if small:
        operands = [pltpu.with_memory_space_constraint(x, pltpu.HBM) for x in operands]
        outs += [jax.ShapeDtypeStruct((features, tokens // 2), BF16)]
        outs += [jax.ShapeDtypeStruct((2, 1, units), F32)] * 2 + [jax.ShapeDtypeStruct((1, features), F32)]
    outs = pl.pallas_call(
        fetching_kernel if small else products_kernel,
        out_shape=outs,
        in_specs=[HBM if small else VMEM] * len(operands),
        out_specs=[VMEM] * len(outs),
        scratch_shapes=scratch if small else scratch[:1],
        compiler_params=PARAMS,
        cost_estimate=pl.CostEstimate(
            flops=2 * tokens * features * columns, bytes_accessed=4 * features * columns, transcendentals=0
        ),
    )(*operands)
    return outs[:SIDE], outs[SIDE:]


def total_of(refs):
    return sum(ref[...].astype(F32) for ref in refs[1:]) + refs[0][...].astype(F32)


def add_kernel(*refs):
    *in_refs, out_ref = refs
    end = out_ref.shape[0] - 8
    total = total_of(in_refs)
    out_ref[:end] = total[:end].astype(BF16)
    squares = whole_squares(total[end:])
    high = squares.astype(BF16).astype(F32)
    lane = lax.broadcasted_iota(jnp.int32, squares.shape, 1)
    out_ref[end:] = jnp.where(lane % 2 == 0, high, pltpu.roll(squares - high, 1, 1)).astype(BF16)


def hidden_kernel(count, *refs):
    in_refs, scales_refs, out_ref = refs[:SIDE], refs[SIDE : SIDE + count], refs[-1]
    rows, units = out_ref.shape
    each = units // count
    total = total_of(in_refs)
    inverse = lax.rsqrt(whole_squares(total[2 * units // 128 * rows :]) / D + 1e-06)
    inverse = jnp.concatenate([inverse[:, 2 * k : 2 * k + 1] for k in range(rows // 8)])
    for n in range(units // 128):
        scales_ref, at = scales_refs[n * 128 // each], n * 128 % each
        gate = inverse * scales_ref[0, :, at : at + 128] * total[n * rows : (n + 1) * rows]
        m = n + units // 128
        up = inverse * scales_ref[1, :, at : at + 128] * total[m * rows : (m + 1) * rows]
        out_ref[:, n * 128 : (n + 1) * 128] = (gate / (1.0 + jnp.exp(-gate)) * up).astype(BF16)


def down_kernel(count, *refs):
    in_refs, w_refs, (*out_refs, hidden) = refs[:SIDE], refs[SIDE : SIDE + count], refs[SIDE + count :]
    rows = in_refs[0].shape[0]
    tokens = rows * SIDE
    place = place_in_f()
    turn = lax.axis_index("cb") % 2 * (SIDE // 2) if len(out_refs) == 2 else 0
    for k, ref in enumerate(in_refs):
        at = pl.multiple_of(((place ^ k) + turn) % SIDE * rows, rows)
        hidden[pl.ds(at, rows)] = ref[...]
    each = hidden.shape[1] // count
    for n, out_ref in enumerate(out_refs):
        wide = tokens // len(out_refs)
        parts = [
            lax.dot_general(
                w_ref[...].astype(BF16),
                hidden[n * wide : (n + 1) * wide, k * each : (k + 1) * each],
                (((1,), (1,)), ((), ())),
                preferred_element_type=F32,
            )
            for k, w_ref in enumerate(w_refs)
        ]
        out_ref[...] = functools.reduce(jnp.add, parts).astype(BF16)


def call(kernel, shapes, *operands, scratch=(), flops=0):
    return pl.pallas_call(
        kernel,
        out_shape=[jax.ShapeDtypeStruct(shape, BF16) for shape in shapes],
        in_specs=[VMEM] * len(operands),
        out_specs=[VMEM] * len(shapes),
        scratch_shapes=scratch,
        compiler_params=PARAMS,
        cost_estimate=pl.CostEstimate(
            flops=flops or 8 * operands[0].size,
            bytes_accessed=sum(x.size * x.dtype.itemsize for x in operands),
            transcendentals=0,
        ),
    )(*operands)


def hidden_blocks(mine, scales):
    peers = [swapped(mine, k, False) for k in ORDER]
    units = sum(x.shape[2] for x in scales)
    rows = mine.shape[0] // (2 * units // 128)
    kernel = functools.partial(hidden_kernel, len(scales))
    (hidden,) = call(kernel, [(rows, units)], mine, *peers, *scales)
    others = {k: swapped(hidden, k, True) for k in G_ORDER}
    return hidden, others[1], others[2], others[3]


def down_products(blocks, weights, outs):
    rows, units = blocks[0].shape
    tokens, features = rows * SIDE, weights[0].shape[1]
    return call(
        functools.partial(down_kernel, len(weights)),
        [(features, tokens // outs)] * outs,
        *blocks,
        *(w.T for w in weights),
        scratch=[pltpu.VMEM((tokens, units), BF16)],
        flops=2 * tokens * units * features,
    )


def step_result(stream, down_scale, down):
    return (stream.astype(F32) + 0.5 * down_scale[:, None] * down).astype(BF16)


def body(
    tokens,
    first_gain,
    first_gate,
    first_up,
    first_down,
    first_gate_scale,
    first_up_scale,
    first_down_scale,
    second_gain,
    second_gate,
    second_up,
    second_down,
    second_gate_scale,
    second_up_scale,
    second_down_scale,
):
    small = (first_gate_scale, first_up_scale, second_gate_scale, second_up_scale, second_gain)
    blocks, (half, scales, later_scales, later_gain) = products(
        tokens.T, first_gain[None, :], (first_gate, first_up), [x[None, :] for x in small]
    )
    received = [swapped(blocks[k], k, True) for k in ORDER]
    theirs = [other_core(x) for x in (second_gate, second_up, second_down.T, later_scales)]
    received, theirs = lax.optimization_barrier((received, theirs))
    their_gate, their_up, their_down, their_scales = theirs
    (mine,) = call(add_kernel, [blocks[0].shape], blocks[0], *received)
    near, far = down_products(hidden_blocks(mine, [scales]), [first_down], 2)
    chip = rounded(near.astype(F32) + other_core(far).astype(F32))
    middle = step_result(half, first_down_scale, sum_over_x(chip))

    blocks, _ = products(middle, later_gain, (second_gate, their_gate, second_up, their_up))
    received = [swapped(blocks[k], k, True) for k in ORDER]
    (mine,) = call(add_kernel, [blocks[0].shape], blocks[0], *received)
    hidden = hidden_blocks(mine, [later_scales, their_scales])
    (down,) = down_products(hidden, [second_down, their_down.T], 1)
    mixed = step_result(middle, second_down_scale, sum_over_x(down.astype(F32)))
    other = other_core(mixed)
    first = lax.axis_index("cb") % 2 == 0
    both = jnp.where(first, jnp.concatenate([mixed, other], axis=1), jnp.concatenate([other, mixed], axis=1))
    return both.T


def solution(mesh):
    one = (P("ra"), P("ra", "cb"), P("ra", "cb"), P("cb", "ra"), P("cb"), P("cb"), P("ra"))
    return jax.shard_map(
        body, mesh=mesh, in_specs=(P(None, "ra"), *one, *one), out_specs=P(None, "ra"), check_vma=False
    )
```
